32 devices in a mesh: ep: 4 (over z), tp: 8 (over y, x, core).
Axes of the slice: x: 2, y: 2, z: 4, core: 2. Of those that a mesh axis runs over, the one named last changes fastest.
Arguments:
- hidden: bfloat16 [64, 4096], P('ep', 'tp'), may hold values from -6 to 6
- norm_gain: float32 [4096], replicated, may hold values from 0.1 to 1.9
- routes: int32 [64, 4], P('ep'), may hold values from 0 to 7, all different within a row; in each aligned block of 16 rows (0 to 15, 16 to 31, ...) at most 13 rows name the same one
- route_weights: float32 [64, 4], P('ep'), may hold values from 0.1 to 1
- gate_weight: bfloat16 [8, 1024, 4096], P('ep', 'tp'), may hold values from -0.09375 to 0.09375
- up_weight: bfloat16 [8, 1024, 4096], P('ep', 'tp'), may hold values from -0.09375 to 0.09375
- down_weight: bfloat16 [8, 1024, 4096], P('ep', 'tp'), may hold values from -0.25 to 0.25
- shared_gate: bfloat16 [1024, 4096], P('tp'), may hold values from -0.09375 to 0.09375
- shared_up: bfloat16 [1024, 4096], P('tp'), may hold values from -0.09375 to 0.09375
- shared_down: bfloat16 [1024, 4096], P('tp'), may hold values from -0.25 to 0.25
Outputs:
- mixed: bfloat16 [64, 4096], P('ep', 'tp')
The draws below stay inside these ranges and needn't reach their ends.
Inputs may be any that keep to these rules, and one draw needn't show every extreme that they name: `routes`: each row names 4 different experts; among the rows of one index of ep (aligned blocks of 16 rows) no expert is named more than 13 times, a bound that some block reaches.
All inputs are finite; a program needn't handle non-finite values.
Results may differ from the reference program's by a relative error of at most 0.017.
Values may be sent and summed in bfloat16 or wider, within the bound.
A program may use at most 64 MiB of HBM per device.

```python
import math
import jax
import jax.numpy as jnp
import numpy as np
from jax import lax

D = 4096
FF = 1024
FFS = 1024
TOP_K = 4
TOK_DEV = 16
EXPERTS = 8
CAP = 13
TOKENS = 64
N_EP = 4
N_TP = 8


def with_spikes(values, rng, source, target, blocks, factor):
    owner, partner = [(jnp.arange(values.shape[dim]) // (values.shape[dim] // blocks)).reshape([-1 if axis == dim else 1 for axis in range(values.ndim)]) for dim in (source, target)]
    chosen = jax.random.permutation(rng, blocks)[partner]
    strong = (owner == chosen) | (owner == (partner + blocks // 2) % blocks)
    return jnp.where(strong, factor * values, values)


def levels(own_key, extent, shards, smallest, largest):
    def one(axis_at, shards_of):
        heights = jax.random.uniform(jax.random.fold_in(jax.random.fold_in(own_key, 6), axis_at), (shards_of,), jnp.float32, smallest / len(shards), largest / len(shards))
        return jnp.repeat(jnp.exp(heights), extent[axis_at] // shards_of).reshape((-1,) + (1,) * (len(extent) - axis_at - 1))

    gain = one(*shards[0])
    for cut in shards[1:]:
        gain = gain * one(*cut)
    return gain


def shared_out(stream_key, own, number, rows, number_of, top, limit, lean):
    order = jax.random.permutation(stream_key, number_of)
    crowded, ordinary = shares(number_of, rows * top, limit, lean, True), shares(number_of, rows * top, limit, lean, False)
    places = jnp.arange(number_of)

    def named(sizes, rotation):
        used = int((sizes > 0).sum())
        fixed = max(1, used // 4)
        shifted = fixed + (places - fixed + rotation * (used - fixed)) % max(1, number_of - fixed)
        return jnp.zeros((number_of,), jnp.int32).at[order[jnp.where(places < fixed, places, shifted)]].set(jnp.asarray(sizes, jnp.int32))

    sizes = jnp.where(number % 4 == 0, named(crowded, number // 4), named(ordinary, number - number // 4 - 1))
    mixed = jax.random.permutation(jax.random.fold_in(own, 3), number_of)
    source_of, taker = mixed[0:number_of // 2 * 2:2], mixed[1:number_of // 2 * 2:2]
    margin = jnp.minimum(sizes[source_of] - 1, limit - sizes[taker]) // 2
    margin = jnp.where((source_of == order[0]) | (taker == order[0]) | (sizes[taker] == 0), 0, jnp.maximum(margin, 0))
    shifted = jax.random.randint(jax.random.fold_in(own, 4), (number_of // 2,), 0, 1 << 20) % (margin + 1)
    sizes = sizes.at[source_of].add(-shifted).at[taker].add(shifted)
    members = jnp.searchsorted(jnp.cumsum(sizes), jnp.arange(rows * top), side="right").astype(jnp.int32)
    grid = members.reshape(top, rows).T
    grid = grid[jax.random.permutation(jax.random.fold_in(own, 1), rows)]
    rotation = jax.random.randint(jax.random.fold_in(own, 2), (rows, 1), 0, top)
    return jnp.take_along_axis(grid, (jnp.arange(top)[None, :] + rotation) % top, axis=1)


def shares(amount, total, limit, slope, full):
    portions = [(1 << 20) // math.isqrt(grade ** slope) + 1 for grade in range(1, amount + 1)]
    largest = limit if full else min(limit, max(-(-total // amount), total * portions[0] // sum(portions)))
    least = 1 if total - largest >= amount - 1 else 0
    holding, rest = [largest] + [least] * (amount - 1), total - largest - least * (amount - 1)
    while rest > 0:
        candidates = [i for i in range(1, amount) if holding[i] < largest] or [i for i in range(1, amount) if holding[i] < limit]
        mass, remaining = sum([portions[i] for i in candidates]), rest
        for i in candidates:
            more = min(limit - holding[i], max(1, remaining * portions[i] // mass), rest)
            holding[i] = holding[i] + more
            rest = rest - more
    return np.array(holding)


def noise(rng, shape, deviation, bound, pieces=(), held_as=jnp.bfloat16):
    result = jax.random.normal(rng, shape, jnp.float32) * deviation
    if len(pieces) > 0:
        result = levels(rng, shape, pieces, -0.22, 0.18) * result
    return jnp.clip(result, min=-bound, max=bound).astype(held_as)


def heavy_noise(rng, shape, deviation, limit, pieces, heavy, kind=jnp.bfloat16):
    drawn = deviation * jax.random.normal(rng, shape, jnp.float32)
    if pieces:
        drawn = drawn * levels(rng, shape, pieces, -0.22, 0.18)
    return jnp.clip(with_spikes(drawn, jax.random.fold_in(rng, 3), *heavy), -limit, limit).astype(kind)


def setup_inputs(seed: int = 0) -> dict:
    streams_of = jax.random.split(jax.random.key(seed), 11)
    hidden = noise(streams_of[0], (TOKENS, D), 1.0, 6.0, ((0, 4), (1, 8)))
    norm_gain = jnp.clip(1.0 + 0.18 * jax.random.normal(streams_of[1], (D,), jnp.float32), 0.1, 1.9)
    routes_keys = jax.random.split(jax.random.fold_in(streams_of[2], 1), TOKENS // TOK_DEV)
    routes_turns = jax.random.permutation(jax.random.fold_in(streams_of[2], 3), TOKENS // TOK_DEV)
    routes = jax.vmap(lambda own, number: shared_out(jax.random.fold_in(streams_of[2], 2), own, number, TOK_DEV, EXPERTS, TOP_K, CAP, 2))(routes_keys, routes_turns).reshape((TOKENS, TOP_K))
    route_weights = jnp.clip(jnp.exp(math.log(1.0) - 2.3025851 * jax.random.uniform(streams_of[3], (TOKENS, TOP_K), jnp.float32) ** levels(streams_of[3], (TOKENS, TOP_K), ((0, 4),), -0.2, 0.2)), 0.1, 1.0)
    gate_weight = noise(streams_of[4], (EXPERTS, FF, D), D ** -0.5, 0.09375, ((0, 4), (1, 8)))
    up_weight = noise(streams_of[5], (EXPERTS, FF, D), D ** -0.5, 0.09375, ((0, 4), (1, 8)))
    down_weight = heavy_noise(streams_of[6], (EXPERTS, FF, D), FF ** -0.5, 0.25, ((0, 4), (1, 8)), (1, 2, 8, 2.0))
    shared_gate = noise(streams_of[7], (FFS, D), D ** -0.5, 0.09375, ((0, 8),))
    shared_up = noise(streams_of[8], (FFS, D), D ** -0.5, 0.09375, ((0, 8),))
    shared_down = heavy_noise(streams_of[9], (FFS, D), FFS ** -0.5, 0.25, ((0, 8),), (0, 1, 8, 2.0))
    return dict(hidden=hidden, norm_gain=norm_gain, routes=routes, route_weights=route_weights, gate_weight=gate_weight, up_weight=up_weight, down_weight=down_weight, shared_gate=shared_gate, shared_up=shared_up, shared_down=shared_down)


norm_eps = 1e-06

def norm_rows(hidden, norm_gain):
    values = hidden.astype(jnp.float32)
    inv_scale = lax.rsqrt(lax.optimization_barrier(jnp.mean(values * values, axis=-1, keepdims=True)) + norm_eps)
    return (values * inv_scale * norm_gain.astype(jnp.float32)).astype(jnp.bfloat16)

def slot_table(route_block):
    onehot = (route_block[:, :, None] == jnp.arange(EXPERTS, dtype=jnp.int32)[None, None, :]).astype(jnp.int32)
    used_mask = lax.optimization_barrier(jnp.sum(onehot, axis=1))
    before = jnp.cumsum(used_mask, axis=0) - used_mask
    slot_rank = lax.optimization_barrier(jnp.sum(onehot * before[:, None, :], axis=2))
    return (route_block * CAP + slot_rank).astype(jnp.int32)

def block_partials(inner_vals, down_w):
    row_count = inner_vals.shape[0]
    part_sums = jnp.einsum('rpf,pfd->rpd', inner_vals.reshape(row_count, N_TP, -1).astype(jnp.float32), down_w.reshape(N_TP, -1, D).astype(jnp.float32), precision=lax.Precision.HIGHEST)
    rounded = lax.optimization_barrier(part_sums.astype(jnp.bfloat16))
    return lax.optimization_barrier(jnp.sum(rounded.astype(jnp.float32), axis=1))

def expert_rows(row_block, gate_one, up_one, down_one):
    dims = (((1,), (1,)), ((), ()))
    gate_vals = lax.dot_general(row_block, gate_one, dims, preferred_element_type=jnp.float32)
    up_vals = lax.dot_general(row_block, up_one, dims, preferred_element_type=jnp.float32)
    inner_vals = (jax.nn.silu(gate_vals) * up_vals).astype(jnp.bfloat16)
    return block_partials(inner_vals, down_one)

def reference(hidden, norm_gain, routes, route_weights, gate_weight, up_weight, down_weight, shared_gate, shared_up, shared_down):
    normed = norm_rows(hidden, norm_gain)
    token_blocks = normed.reshape(N_EP, TOK_DEV, D)
    route_blocks = routes.reshape(N_EP, TOK_DEV, TOP_K)
    weight_blocks = route_weights.reshape(N_EP, TOK_DEV, TOP_K)
    slot_ids = jax.vmap(slot_table)(route_blocks)
    slot_range = jnp.arange(EXPERTS * CAP, dtype=jnp.int32)
    matches = slot_ids[:, :, :, None] == slot_range[None, None, None, :]
    select = lax.optimization_barrier(jnp.sum(matches.astype(jnp.float32), axis=2))
    combine = lax.optimization_barrier(jnp.sum(jnp.where(matches, weight_blocks[:, :, :, None], 0.0), axis=2))
    buffer = jnp.einsum('btr,btd->brd', select, token_blocks.astype(jnp.float32), precision=lax.Precision.HIGHEST).astype(jnp.bfloat16)
    buffer = buffer.reshape(N_EP, EXPERTS, CAP, D).transpose(1, 0, 2, 3).reshape(EXPERTS, N_EP * CAP, D)

    def one_expert(operands):
        row_block, gate_one, up_one, down_one = operands
        return expert_rows(row_block, gate_one, up_one, down_one).astype(jnp.bfloat16)
    expert_out = lax.map(one_expert, (buffer, gate_weight, up_weight, down_weight))
    expert_out = expert_out.reshape(EXPERTS, N_EP, CAP, D).transpose(1, 0, 2, 3).reshape(N_EP, EXPERTS * CAP, D)
    routed = jnp.einsum('btr,brd->btd', combine, expert_out.astype(jnp.float32), precision=lax.Precision.HIGHEST).reshape(TOKENS, D)
    shared = expert_rows(normed, shared_gate, shared_up, shared_down)
    return (routed + shared).astype(jnp.bfloat16)
```

```python
import functools

import jax
import jax.numpy as jnp
from jax import lax
from jax.experimental import pallas as pl
from jax.experimental.pallas import tpu as pltpu
from jax.sharding import PartitionSpec as P

MESH = pl.DeviceIdType.MESH
norm_eps = 1e-06
NT = (((1,), (1,)), ((), ()))
F32 = jnp.float32
BF16 = jnp.bfloat16


def flip(index, bits, count):
    if count & (count - 1):
        return lax.rem(index + bits, count)
    result, place = 0, 1
    while place < count:
        digit = lax.rem(index // place, 2)
        if (bits // place) % 2:
            digit = 1 - digit
        result = result + digit * place
        place *= 2
    return result


def unflip(index, bits, count):
    if count & (count - 1):
        return lax.rem(index + count - bits, count)
    return flip(index, bits, count)


def far_first(count):
    return sorted(range(count), key=lambda step: -min(step, count - step))


def kernel(
    groups,
    width,
    cores,
    shared_split,
    hidden_hbm,
    gain_hbm,
    routes_hbm,
    rw_hbm,
    gate_hbm,
    up_hbm,
    down_hbm,
    sgate_hbm,
    sup_hbm,
    sdown_hbm,
    out_ref,
    xbuf,
    gain,
    routes,
    rw,
    table,
    gate_w,
    up_w,
    down_w,
    sgate_w,
    sup_w,
    sdown_w,
    acc_g,
    acc_u,
    acc_sg,
    acc_su,
    acc_ss,
    core_send,
    core_recv,
    plane_send,
    plane_recv,
    total,
    z_send,
    z_recv,
    load_sem,
    zs_sem,
    zr_sem,
    ts_sem,
    tr_sem,
    ps_sem,
    pr_sem,
    ds_sem,
    dr_sem,
    cs_sem,
    cr_sem,
    qs_sem,
    qr_sem,
    ys_sem,
    yr_sem,
):
    e = lax.axis_index("ep")
    p = lax.axis_index("tp")
    chips = width // cores
    q, c = p // cores, lax.rem(p, cores)
    rows, feats = hidden_hbm.shape
    tokens = rows * groups
    local, units, _ = gate_hbm.shape
    split_units = sgate_w.shape[0]

    def at_chip(chip, core):
        return chip * cores + core

    def block(index):
        return pl.ds(pl.multiple_of(index * rows, rows), rows)

    def columns(index):
        return pl.ds(pl.multiple_of(index * feats, feats), feats)

    loads = [
        pltpu.make_async_copy(hidden_hbm, xbuf.at[p, block(e)], load_sem.at[0]),
        pltpu.make_async_copy(routes_hbm, routes, load_sem.at[1]),
        pltpu.make_async_copy(rw_hbm, rw, load_sem.at[2]),
        pltpu.make_async_copy(gain_hbm, gain, load_sem.at[3]),
    ]
    part = pl.ds(
        pl.multiple_of(e * split_units, split_units) if shared_split else 0, split_units
    )
    number = len(loads)
    for index in range(local):
        span = pl.ds(index * units, units)
        for source, target in ((gate_hbm, gate_w), (up_hbm, up_w)):
            loads.append(
                pltpu.make_async_copy(source.at[index], target.at[span], load_sem.at[len(loads)])
            )
    for source, target in ((sgate_hbm, sgate_w), (sup_hbm, sup_w)):
        loads.append(pltpu.make_async_copy(source.at[part], target, load_sem.at[len(loads)]))
    first_done = len(loads)
    for index in range(local):
        span = pl.ds(index * units, units)
        loads.append(
            pltpu.make_async_copy(down_hbm.at[index], down_w.at[span], load_sem.at[len(loads)])
        )
    loads.append(pltpu.make_async_copy(sdown_hbm.at[part], sdown_w, load_sem.at[len(loads)]))
    for load in loads:
        load.start()

    barrier = pltpu.get_barrier_semaphore()
    partners = [(lax.rem(e + step, groups), p) for step in range(1, groups)]
    partners += [(e, at_chip(flip(q, d, chips), c)) for d in range(1, chips)]
    partners += [(e, at_chip(q, lax.rem(c + step, cores))) for step in range(1, cores)]
    for partner in partners:
        pl.semaphore_signal(barrier, inc=1, device_id=partner, device_id_type=MESH)

    loads[1].wait()
    loads[2].wait()
    lane = lax.broadcasted_iota(jnp.int32, (rows, table.shape[2]), 1)
    dense = jnp.zeros((rows, table.shape[2]), F32)
    for k in range(routes.shape[1]):
        dense = dense + jnp.where(lane == routes[:, k : k + 1], rw[:, k : k + 1], 0.0)
    table[e] = dense
    loads[0].wait()
    pl.semaphore_wait(barrier, len(partners))

    sends = []

    def remote(source, target, send, recv, device, go=True):
        copy = pltpu.make_async_remote_copy(
            src_ref=source,
            dst_ref=target,
            send_sem=send,
            recv_sem=recv,
            device_id=device,
            device_id_type=MESH,
        )
        if go:
            copy.start()
            sends.append(copy)
        return copy

    for step in far_first(groups):
        if step:
            mine = xbuf.at[p, block(e)]
            remote(mine, mine, zs_sem.at[step], zr_sem.at[step], (lax.rem(e + step, groups), p))
    if groups * chips <= 32:
        pieces = [[step] for step in [0] + far_first(groups)[::-1] if step or True]
        pieces = [[0]] + [[step] for step in far_first(groups)[::-1] if step]
    else:
        pieces = [list(range(groups))]

    def piece_rows(piece):
        if len(piece) > 1:
            return pl.ds(0, tokens)
        return block(lax.rem(e + groups - piece[0], groups))

    core_next = lax.rem(c + 1, cores)
    for number, piece in enumerate(pieces):
        for step in piece:
            if step:
                theirs = xbuf.at[p, block(lax.rem(e + groups - step, groups))]
                remote(theirs, theirs, zs_sem.at[step], zr_sem.at[step], (e, p), False).wait_recv()
        view = xbuf.at[p, piece_rows(piece)]
        for d in range(chips - 1, 0, -1):
            remote(
                view,
                view,
                ps_sem.at[number, d],
                pr_sem.at[number, d],
                (e, at_chip(flip(q, d, chips), c)),
            )
        remote(view, view, ds_sem.at[number, 0], dr_sem.at[number, 0], (e, at_chip(q, core_next)))
        if number == 0:
            for step in far_first(groups):
                if step:
                    remote(
                        table.at[e],
                        table.at[e],
                        ts_sem.at[step],
                        tr_sem.at[step],
                        (lax.rem(e + step, groups), p),
                    )

    def project(owner, first):
        values = xbuf[owner].astype(F32)
        scaled = (values * gain[:, columns(owner)]).astype(BF16)
        squares = values * values
        partial = squares[:, :128]
        for start in range(128, feats, 128):
            partial = partial + squares[:, start : start + 128]
        for acc, weight in (
            (acc_g, gate_w),
            (acc_u, up_w),
            (acc_sg, sgate_w),
            (acc_su, sup_w),
        ):
            product = lax.dot_general(
                scaled, weight[:, columns(owner)], NT, preferred_element_type=F32
            )
            acc[...] = product if first else acc[...] + product
        acc_ss[...] = partial if first else acc_ss[...] + partial

    for load in loads[3:first_done]:
        load.wait()
    project(p, True)

    for d in range(1, chips):
        owner = at_chip(unflip(q, d, chips), c)
        for number, piece in enumerate(pieces):
            view = xbuf.at[owner, piece_rows(piece)]
            remote(view, view, ps_sem.at[number, d], pr_sem.at[number, d], (e, p), False).wait_recv()
            remote(
                view, view, ds_sem.at[number, d], dr_sem.at[number, d], (e, at_chip(q, core_next))
            )
        project(owner, False)
    for d in range(chips):
        owner = at_chip(unflip(q, d, chips), core_next)
        for number, piece in enumerate(pieces):
            view = xbuf.at[owner, piece_rows(piece)]
            remote(view, view, ds_sem.at[number, d], dr_sem.at[number, d], (e, p), False).wait_recv()
        project(owner, False)

    for step in range(1, groups):
        theirs = table.at[lax.rem(e + groups - step, groups)]
        remote(theirs, theirs, ts_sem.at[step], tr_sem.at[step], (e, p), False).wait_recv()

    inv = lax.rsqrt(jnp.sum(acc_ss[...], axis=1, keepdims=True) / (feats * width) + norm_eps)
    tables = table[...].reshape(tokens, table.shape[2])
    lanes = lax.broadcasted_iota(jnp.int32, tables.shape, 1)
    unit = lax.broadcasted_iota(jnp.int32, (tokens, local * units), 1)
    mix = jnp.zeros((tokens, local * units), F32)
    for index in range(local):
        mine = jnp.sum(
            jnp.where(lanes == e * local + index, tables, 0.0), axis=1, keepdims=True
        )
        inside = (unit >= index * units) & (unit < (index + 1) * units)
        mix = jnp.where(inside, mine, mix)

    def swish(v):
        return v / (1.0 + jnp.exp(-v))

    inner = (swish(acc_g[...] * inv) * (acc_u[...] * inv) * mix).astype(BF16)
    shared = swish(acc_sg[...] * inv) * (acc_su[...] * inv)
    if not shared_split:
        row = lax.broadcasted_iota(jnp.int32, shared.shape, 0)
        shared = jnp.where((row >= e * rows) & (row < (e + 1) * rows), shared, 0.0)
    shared = shared.astype(BF16)
    for load in loads[first_done:]:
        load.wait()

    def expand(owner):
        return jnp.dot(
            inner, down_w[:, columns(owner)], preferred_element_type=F32
        ) + jnp.dot(shared, sdown_w[:, columns(owner)], preferred_element_type=F32)

    order = list(range(chips - 1, -1, -1))
    for d in order:
        core_send[d] = expand(at_chip(flip(q, d, chips), core_next)).astype(BF16)
        remote(
            core_send.at[d], core_recv.at[d], cs_sem.at[d], cr_sem.at[d], (e, at_chip(q, core_next))
        )
    if len(pieces) > 1:
        out_pieces = [[step] for step in far_first(groups)]
    else:
        out_pieces = pieces

    def out_rows(piece):
        if len(piece) > 1:
            return pl.ds(0, tokens)
        return block(lax.rem(e + piece[0], groups))

    for d in order:
        value = expand(at_chip(flip(q, d, chips), c))
        remote(
            core_send.at[d], core_recv.at[d], cs_sem.at[d], cr_sem.at[d], (e, p), False
        ).wait_recv()
        value = value + core_recv[d].astype(F32)
        if d == 0:
            total[...] = value
        else:
            plane_send[d] = value.astype(BF16)
            for number, piece in enumerate(out_pieces):
                remote(
                    plane_send.at[d, out_rows(piece)],
                    plane_recv.at[d, out_rows(piece)],
                    qs_sem.at[number, d],
                    qr_sem.at[number, d],
                    (e, at_chip(flip(q, d, chips), c)),
                )
    for number, piece in enumerate(out_pieces):
        for d in range(1, chips):
            view = plane_recv.at[d, out_rows(piece)]
            remote(view, view, qs_sem.at[number, d], qr_sem.at[number, d], (e, p), False).wait_recv()
        for step in piece:
            span = block(lax.rem(e + step, groups))
            value = total[span, :]
            for d in range(1, chips):
                value = value + plane_recv[d, span, :].astype(F32)
            if step:
                z_send[step] = value.astype(BF16)
                remote(
                    z_send.at[step],
                    z_recv.at[step],
                    ys_sem.at[step],
                    yr_sem.at[step],
                    (lax.rem(e + step, groups), p),
                )
            else:
                total[span, :] = value
    answer = total[block(e), :]
    for step in range(1, groups):
        remote(
            z_send.at[step], z_recv.at[step], ys_sem.at[step], yr_sem.at[step], (e, p), False
        ).wait_recv()
        answer = answer + z_recv[step].astype(F32)
    out_ref[...] = answer.astype(BF16)
    for copy in sends:
        copy.wait_send()


def solution(mesh):
    groups, width = mesh.shape["ep"], mesh.shape["tp"]
    cores = 2

    def step(hidden, gain, routes, rw, gate, up, down, sgate, sup, sdown):
        rows, feats = hidden.shape
        local, units, model = gate.shape
        tokens = rows * groups
        chips = width // cores
        shared_units = sgate.shape[0]
        shared_split = shared_units % (16 * groups) == 0
        split_units = shared_units // groups if shared_split else shared_units
        lanes = -(-local * groups // 128) * 128
        count = groups if groups * chips <= 32 else 1
        dma = pltpu.SemaphoreType.DMA
        any_spec = pl.BlockSpec(memory_space=pl.ANY)
        return pl.pallas_call(
            functools.partial(kernel, groups, width, cores, shared_split),
            out_shape=jax.ShapeDtypeStruct((rows, feats), BF16),
            in_specs=[any_spec] * 10,
            out_specs=pl.BlockSpec(memory_space=pltpu.VMEM),
            scratch_shapes=[
                pltpu.VMEM((width, tokens, feats), BF16),
                pltpu.VMEM((1, model), F32),
                pltpu.VMEM(routes.shape, jnp.int32),
                pltpu.VMEM(rw.shape, F32),
                pltpu.VMEM((groups, rows, lanes), F32),
                pltpu.VMEM((local * units, model), BF16),
                pltpu.VMEM((local * units, model), BF16),
                pltpu.VMEM((local * units, model), BF16),
                pltpu.VMEM((split_units, model), BF16),
                pltpu.VMEM((split_units, model), BF16),
                pltpu.VMEM((split_units, model), BF16),
                pltpu.VMEM((tokens, local * units), F32),
                pltpu.VMEM((tokens, local * units), F32),
                pltpu.VMEM((tokens, split_units), F32),
                pltpu.VMEM((tokens, split_units), F32),
                pltpu.VMEM((tokens, 128), F32),
                pltpu.VMEM((chips, tokens, feats), BF16),
                pltpu.VMEM((chips, tokens, feats), BF16),
                pltpu.VMEM((chips, tokens, feats), BF16),
                pltpu.VMEM((chips, tokens, feats), BF16),
                pltpu.VMEM((tokens, feats), F32),
                pltpu.VMEM((groups, rows, feats), BF16),
                pltpu.VMEM((groups, rows, feats), BF16),
                dma((4 + 3 * local + 3,)),
                dma((groups,)),
                dma((groups,)),
                dma((groups,)),
                dma((groups,)),
                dma((count, chips)),
                dma((count, chips)),
                dma((count, chips)),
                dma((count, chips)),
                dma((chips,)),
                dma((chips,)),
                dma((count, chips)),
                dma((count, chips)),
                dma((groups,)),
                dma((groups,)),
            ],
            compiler_params=pltpu.CompilerParams(
                collective_id=0,
                has_side_effects=True,
                vmem_limit_bytes=60 * 1024 * 1024,
            ),
            name="moe_step",
        )(hidden, gain.reshape(1, -1), routes, rw, gate, up, down, sgate, sup, sdown)

    in_specs = (
        P("ep", "tp"),
        P(),
        P("ep", None),
        P("ep", None),
        P("ep", "tp", None),
        P("ep", "tp", None),
        P("ep", "tp", None),
        P("tp", None),
        P("tp", None),
        P("tp", None),
    )
    return jax.shard_map(
        step, mesh=mesh, in_specs=in_specs, out_specs=P("ep", "tp"), check_vma=False
    )
```

```python
import functools

import jax
import jax.numpy as jnp
from jax import lax
from jax.experimental import pallas as pl
from jax.experimental.pallas import tpu as pltpu
from jax.sharding import PartitionSpec as P

MESH = pl.DeviceIdType.MESH
norm_eps = 1e-06
NT = (((1,), (1,)), ((), ()))
F32 = jnp.float32
BF16 = jnp.bfloat16


def flip(index, bits, count):
    if count & (count - 1):
        return lax.rem(index + bits, count)
    result, place = 0, 1
    while place < count:
        digit = lax.rem(index // place, 2)
        if (bits // place) % 2:
            digit = 1 - digit
        result = result + digit * place
        place *= 2
    return result


def unflip(index, bits, count):
    if count & (count - 1):
        return lax.rem(index + count - bits, count)
    return flip(index, bits, count)


def far_first(count):
    return sorted(range(count), key=lambda step: -min(step, count - step))


def kernel(
    groups,
    width,
    cores,
    shared_split,
    hidden_hbm,
    gain_hbm,
    routes_hbm,
    rw_hbm,
    gate_hbm,
    up_hbm,
    down_hbm,
    sgate_hbm,
    sup_hbm,
    sdown_hbm,
    out_ref,
    xbuf,
    gain,
    routes,
    rw,
    table,
    gate_w,
    up_w,
    down_w,
    sgate_w,
    sup_w,
    sdown_w,
    acc_g,
    acc_u,
    acc_sg,
    acc_su,
    acc_ss,
    core_send,
    core_recv,
    plane_send,
    plane_recv,
    total,
    z_send,
    z_recv,
    load_sem,
    zs_sem,
    zr_sem,
    ts_sem,
    tr_sem,
    ps_sem,
    pr_sem,
    ds_sem,
    dr_sem,
    cs_sem,
    cr_sem,
    qs_sem,
    qr_sem,
    ys_sem,
    yr_sem,
):
    e = lax.axis_index("ep")
    p = lax.axis_index("tp")
    chips = width // cores
    q, c = p // cores, lax.rem(p, cores)
    rows, feats = hidden_hbm.shape
    tokens = rows * groups
    local, units, _ = gate_hbm.shape
    split_units = sgate_w.shape[0]

    def at_chip(chip, core):
        return chip * cores + core

    def block(index):
        return pl.ds(pl.multiple_of(index * rows, rows), rows)

    def columns(index):
        return pl.ds(pl.multiple_of(index * feats, feats), feats)

    loads = [
        pltpu.make_async_copy(hidden_hbm, xbuf.at[p, block(e)], load_sem.at[0]),
        pltpu.make_async_copy(routes_hbm, routes, load_sem.at[1]),
        pltpu.make_async_copy(rw_hbm, rw, load_sem.at[2]),
        pltpu.make_async_copy(gain_hbm, gain, load_sem.at[3]),
    ]
    part = pl.ds(
        pl.multiple_of(e * split_units, split_units) if shared_split else 0, split_units
    )
    number = len(loads)
    for index in range(local):
        span = pl.ds(index * units, units)
        for source, target in ((gate_hbm, gate_w), (up_hbm, up_w)):
            loads.append(
                pltpu.make_async_copy(source.at[index], target.at[span], load_sem.at[len(loads)])
            )
    for source, target in ((sgate_hbm, sgate_w), (sup_hbm, sup_w)):
        loads.append(pltpu.make_async_copy(source.at[part], target, load_sem.at[len(loads)]))
    first_done = len(loads)
    for index in range(local):
        span = pl.ds(index * units, units)
        loads.append(
            pltpu.make_async_copy(down_hbm.at[index], down_w.at[span], load_sem.at[len(loads)])
        )
    loads.append(pltpu.make_async_copy(sdown_hbm.at[part], sdown_w, load_sem.at[len(loads)]))
    for load in loads:
        load.start()

    barrier = pltpu.get_barrier_semaphore()
    partners = [(lax.rem(e + step, groups), p) for step in range(1, groups)]
    partners += [(e, at_chip(flip(q, d, chips), c)) for d in range(1, chips)]
    partners += [(e, at_chip(q, lax.rem(c + step, cores))) for step in range(1, cores)]
    for partner in partners:
        pl.semaphore_signal(barrier, inc=1, device_id=partner, device_id_type=MESH)

    loads[1].wait()
    loads[2].wait()
    lane = lax.broadcasted_iota(jnp.int32, (rows, table.shape[2]), 1)
    dense = jnp.zeros((rows, table.shape[2]), F32)
    chosen, strength = jnp.transpose(routes[...]), jnp.transpose(rw[...])
    for k in range(routes.shape[0]):
        dense = dense + jnp.where(lane == chosen[:, k : k + 1], strength[:, k : k + 1], 0.0)
    table[e] = dense
    loads[0].wait()
    pl.semaphore_wait(barrier, len(partners))

    sends = []

    def remote(source, target, send, recv, device, go=True):
        copy = pltpu.make_async_remote_copy(
            src_ref=source,
            dst_ref=target,
            send_sem=send,
            recv_sem=recv,
            device_id=device,
            device_id_type=MESH,
        )
        if go:
            copy.start()
            sends.append(copy)
        return copy

    for step in far_first(groups):
        if step:
            mine = xbuf.at[p, block(e)]
            remote(mine, mine, zs_sem.at[step], zr_sem.at[step], (lax.rem(e + step, groups), p))
    if groups * chips <= 32:
        pieces = [[0]] + [[step] for step in far_first(groups)[::-1] if step]
    else:
        pieces = [list(range(groups))]

    def piece_rows(piece):
        if len(piece) > 1:
            return pl.ds(0, tokens)
        return block(lax.rem(e + groups - piece[0], groups))

    core_next = lax.rem(c + 1, cores)
    for number, piece in enumerate(pieces):
        for step in piece:
            if step:
                theirs = xbuf.at[p, block(lax.rem(e + groups - step, groups))]
                remote(theirs, theirs, zs_sem.at[step], zr_sem.at[step], (e, p), False).wait_recv()
        view = xbuf.at[p, piece_rows(piece)]
        for d in range(chips - 1, 0, -1):
            remote(
                view,
                view,
                ps_sem.at[number, d],
                pr_sem.at[number, d],
                (e, at_chip(flip(q, d, chips), c)),
            )
        remote(view, view, ds_sem.at[number, 0], dr_sem.at[number, 0], (e, at_chip(q, core_next)))
        if number == 0:
            for step in far_first(groups):
                if step:
                    remote(
                        table.at[e],
                        table.at[e],
                        ts_sem.at[step],
                        tr_sem.at[step],
                        (lax.rem(e + step, groups), p),
                    )

    def project(owner, first):
        values = xbuf[owner].astype(F32)
        scaled = (values * gain[:, columns(owner)]).astype(BF16)
        squares = values * values
        partial = squares[:, :128]
        for start in range(128, feats, 128):
            partial = partial + squares[:, start : start + 128]
        for acc, weight in (
            (acc_g, gate_w),
            (acc_u, up_w),
            (acc_sg, sgate_w),
            (acc_su, sup_w),
        ):
            product = lax.dot_general(
                scaled, weight[:, columns(owner)], NT, preferred_element_type=F32
            )
            acc[...] = product if first else acc[...] + product
        acc_ss[...] = partial if first else acc_ss[...] + partial

    for load in loads[3:first_done]:
        load.wait()
    project(p, True)

    for d in range(1, chips):
        owner = at_chip(unflip(q, d, chips), c)
        for number, piece in enumerate(pieces):
            view = xbuf.at[owner, piece_rows(piece)]
            remote(view, view, ps_sem.at[number, d], pr_sem.at[number, d], (e, p), False).wait_recv()
            remote(
                view, view, ds_sem.at[number, d], dr_sem.at[number, d], (e, at_chip(q, core_next))
            )
        project(owner, False)
    for d in range(chips):
        owner = at_chip(unflip(q, d, chips), core_next)
        for number, piece in enumerate(pieces):
            view = xbuf.at[owner, piece_rows(piece)]
            remote(view, view, ds_sem.at[number, d], dr_sem.at[number, d], (e, p), False).wait_recv()
        project(owner, False)

    for step in range(1, groups):
        theirs = table.at[lax.rem(e + groups - step, groups)]
        remote(theirs, theirs, ts_sem.at[step], tr_sem.at[step], (e, p), False).wait_recv()

    inv = lax.rsqrt(jnp.sum(acc_ss[...], axis=1, keepdims=True) / (feats * width) + norm_eps)
    tables = table[...].reshape(tokens, table.shape[2])
    lanes = lax.broadcasted_iota(jnp.int32, tables.shape, 1)
    unit = lax.broadcasted_iota(jnp.int32, (tokens, local * units), 1)
    mix = jnp.zeros((tokens, local * units), F32)
    for index in range(local):
        mine = jnp.sum(
            jnp.where(lanes == e * local + index, tables, 0.0), axis=1, keepdims=True
        )
        inside = (unit >= index * units) & (unit < (index + 1) * units)
        mix = jnp.where(inside, mine, mix)

    def swish(v):
        return v / (1.0 + jnp.exp(-v))

    inner = (swish(acc_g[...] * inv) * (acc_u[...] * inv) * mix).astype(BF16)
    shared = swish(acc_sg[...] * inv) * (acc_su[...] * inv)
    if not shared_split:
        row = lax.broadcasted_iota(jnp.int32, shared.shape, 0)
        shared = jnp.where((row >= e * rows) & (row < (e + 1) * rows), shared, 0.0)
    shared = shared.astype(BF16)
    for load in loads[first_done:]:
        load.wait()

    def expand(owner):
        return jnp.dot(
            inner, down_w[:, columns(owner)], preferred_element_type=F32
        ) + jnp.dot(shared, sdown_w[:, columns(owner)], preferred_element_type=F32)

    order = list(range(chips - 1, -1, -1))
    for d in order:
        core_send[d] = expand(at_chip(flip(q, d, chips), core_next)).astype(BF16)
        remote(
            core_send.at[d], core_recv.at[d], cs_sem.at[d], cr_sem.at[d], (e, at_chip(q, core_next))
        )
    if len(pieces) > 1:
        out_pieces = [[step] for step in far_first(groups)]
    else:
        out_pieces = pieces

    def out_rows(piece):
        if len(piece) > 1:
            return pl.ds(0, tokens)
        return block(lax.rem(e + piece[0], groups))

    for d in order:
        value = expand(at_chip(flip(q, d, chips), c))
        remote(
            core_send.at[d], core_recv.at[d], cs_sem.at[d], cr_sem.at[d], (e, p), False
        ).wait_recv()
        value = value + core_recv[d].astype(F32)
        if d == 0:
            total[...] = value
        else:
            plane_send[d] = value.astype(BF16)
            for number, piece in enumerate(out_pieces):
                remote(
                    plane_send.at[d, out_rows(piece)],
                    plane_recv.at[d, out_rows(piece)],
                    qs_sem.at[number, d],
                    qr_sem.at[number, d],
                    (e, at_chip(flip(q, d, chips), c)),
                )
    for number, piece in enumerate(out_pieces):
        for d in range(1, chips):
            view = plane_recv.at[d, out_rows(piece)]
            remote(view, view, qs_sem.at[number, d], qr_sem.at[number, d], (e, p), False).wait_recv()
        for step in piece:
            span = block(lax.rem(e + step, groups))
            value = total[span, :]
            for d in range(1, chips):
                value = value + plane_recv[d, span, :].astype(F32)
            if step:
                z_send[step] = value.astype(BF16)
                remote(
                    z_send.at[step],
                    z_recv.at[step],
                    ys_sem.at[step],
                    yr_sem.at[step],
                    (lax.rem(e + step, groups), p),
                )
            else:
                total[span, :] = value
    answer = total[block(e), :]
    for step in range(1, groups):
        remote(
            z_send.at[step], z_recv.at[step], ys_sem.at[step], yr_sem.at[step], (e, p), False
        ).wait_recv()
        answer = answer + z_recv[step].astype(F32)
    out_ref[...] = answer.astype(BF16)
    for copy in sends:
        copy.wait_send()


def solution(mesh):
    groups, width = mesh.shape["ep"], mesh.shape["tp"]
    cores = 2

    def step(hidden, gain, routes, rw, gate, up, down, sgate, sup, sdown):
        rows, feats = hidden.shape
        local, units, model = gate.shape
        tokens = rows * groups
        chips = width // cores
        shared_units = sgate.shape[0]
        shared_split = shared_units % (16 * groups) == 0
        split_units = shared_units // groups if shared_split else shared_units
        lanes = -(-local * groups // 128) * 128
        count = groups if groups * chips <= 32 else 1
        dma = pltpu.SemaphoreType.DMA
        any_spec = pl.BlockSpec(memory_space=pl.ANY)
        return pl.pallas_call(
            functools.partial(kernel, groups, width, cores, shared_split),
            out_shape=jax.ShapeDtypeStruct((rows, feats), BF16),
            in_specs=[any_spec] * 10,
            out_specs=pl.BlockSpec(memory_space=pltpu.VMEM),
            scratch_shapes=[
                pltpu.VMEM((width, tokens, feats), BF16),
                pltpu.VMEM((1, model), F32),
                pltpu.VMEM(routes.shape[::-1], jnp.int32),
                pltpu.VMEM(rw.shape[::-1], F32),
                pltpu.VMEM((groups, rows, lanes), F32),
                pltpu.VMEM((local * units, model), BF16),
                pltpu.VMEM((local * units, model), BF16),
                pltpu.VMEM((local * units, model), BF16),
                pltpu.VMEM((split_units, model), BF16),
                pltpu.VMEM((split_units, model), BF16),
                pltpu.VMEM((split_units, model), BF16),
                pltpu.VMEM((tokens, local * units), F32),
                pltpu.VMEM((tokens, local * units), F32),
                pltpu.VMEM((tokens, split_units), F32),
                pltpu.VMEM((tokens, split_units), F32),
                pltpu.VMEM((tokens, 128), F32),
                pltpu.VMEM((chips, tokens, feats), BF16),
                pltpu.VMEM((chips, tokens, feats), BF16),
                pltpu.VMEM((chips, tokens, feats), BF16),
                pltpu.VMEM((chips, tokens, feats), BF16),
                pltpu.VMEM((tokens, feats), F32),
                pltpu.VMEM((groups, rows, feats), BF16),
                pltpu.VMEM((groups, rows, feats), BF16),
                dma((4 + 3 * local + 3,)),
                dma((groups,)),
                dma((groups,)),
                dma((groups,)),
                dma((groups,)),
                dma((count, chips)),
                dma((count, chips)),
                dma((count, chips)),
                dma((count, chips)),
                dma((chips,)),
                dma((chips,)),
                dma((count, chips)),
                dma((count, chips)),
                dma((groups,)),
                dma((groups,)),
            ],
            compiler_params=pltpu.CompilerParams(
                collective_id=0,
                has_side_effects=True,
                vmem_limit_bytes=60 * 1024 * 1024,
            ),
            name="moe_step",
        )(hidden, gain.reshape(1, -1), routes.T, rw.T, gate, up, down, sgate, sup, sdown)

    in_specs = (
        P("ep", "tp"),
        P(),
        P("ep", None),
        P("ep", None),
        P("ep", "tp", None),
        P("ep", "tp", None),
        P("ep", "tp", None),
        P("tp", None),
        P("tp", None),
        P("tp", None),
    )
    return jax.shard_map(
        step, mesh=mesh, in_specs=in_specs, out_specs=P("ep", "tp"), check_vma=False
    )
```

```python
import functools

import jax
import jax.numpy as jnp
from jax import lax
from jax.experimental import pallas as pl
from jax.experimental.pallas import tpu as pltpu
from jax.sharding import PartitionSpec as P

MESH = pl.DeviceIdType.MESH
norm_eps = 1e-06
NT = (((1,), (1,)), ((), ()))
F32 = jnp.float32
BF16 = jnp.bfloat16


def flip(index, bits, count):
    if count & (count - 1):
        return lax.rem(index + bits, count)
    result, place = 0, 1
    while place < count:
        digit = lax.rem(index // place, 2)
        if (bits // place) % 2:
            digit = 1 - digit
        result = result + digit * place
        place *= 2
    return result


def unflip(index, bits, count):
    if count & (count - 1):
        return lax.rem(index + count - bits, count)
    return flip(index, bits, count)


def far_first(count):
    return sorted(range(count), key=lambda step: -min(step, count - step))


def kernel(
    groups,
    width,
    cores,
    shared_split,
    hidden_hbm,
    gain_hbm,
    routes_hbm,
    rw_hbm,
    gate_hbm,
    up_hbm,
    down_hbm,
    sgate_hbm,
    sup_hbm,
    sdown_hbm,
    out_ref,
    xbuf,
    gain,
    routes,
    rw,
    table,
    gate_w,
    up_w,
    down_w,
    sgate_w,
    sup_w,
    sdown_w,
    acc_g,
    acc_u,
    acc_sg,
    acc_su,
    acc_ss,
    core_send,
    core_recv,
    plane_send,
    plane_recv,
    total,
    z_send,
    z_recv,
    load_sem,
    zs_sem,
    zr_sem,
    ts_sem,
    tr_sem,
    ps_sem,
    pr_sem,
    ds_sem,
    dr_sem,
    cs_sem,
    cr_sem,
    qs_sem,
    qr_sem,
    ys_sem,
    yr_sem,
):
    e = lax.axis_index("ep")
    p = lax.axis_index("tp")
    chips = width // cores
    q, c = p // cores, lax.rem(p, cores)
    rows, feats = hidden_hbm.shape
    tokens = rows * groups
    local, units, _ = gate_hbm.shape
    split_units = sgate_w.shape[0]

    def at_chip(chip, core):
        return chip * cores + core

    def block(index):
        return pl.ds(pl.multiple_of(index * rows, rows), rows)

    def columns(index):
        return pl.ds(pl.multiple_of(index * feats, feats), feats)

    loads = [
        pltpu.make_async_copy(hidden_hbm, xbuf.at[p, block(e)], load_sem.at[0]),
        pltpu.make_async_copy(routes_hbm, routes, load_sem.at[1]),
        pltpu.make_async_copy(rw_hbm, rw, load_sem.at[2]),
        pltpu.make_async_copy(gain_hbm, gain, load_sem.at[3]),
    ]
    part = pl.ds(
        pl.multiple_of(e * split_units, split_units) if shared_split else 0, split_units
    )
    number = len(loads)
    for index in range(local):
        span = pl.ds(index * units, units)
        for source, target in ((gate_hbm, gate_w), (up_hbm, up_w)):
            loads.append(
                pltpu.make_async_copy(source.at[index], target.at[span], load_sem.at[len(loads)])
            )
    for source, target in ((sgate_hbm, sgate_w), (sup_hbm, sup_w)):
        loads.append(pltpu.make_async_copy(source.at[part], target, load_sem.at[len(loads)]))
    first_done = len(loads)
    for index in range(local):
        span = pl.ds(index * units, units)
        loads.append(
            pltpu.make_async_copy(down_hbm.at[index], down_w.at[span], load_sem.at[len(loads)])
        )
    loads.append(pltpu.make_async_copy(sdown_hbm.at[part], sdown_w, load_sem.at[len(loads)]))
    for load in loads:
        load.start()

    barrier = pltpu.get_barrier_semaphore()
    partners = [(lax.rem(e + step, groups), p) for step in range(1, groups)]
    partners += [(e, at_chip(flip(q, d, chips), c)) for d in range(1, chips)]
    partners += [(e, at_chip(q, lax.rem(c + step, cores))) for step in range(1, cores)]
    for partner in partners:
        pl.semaphore_signal(barrier, inc=1, device_id=partner, device_id_type=MESH)

    loads[1].wait()
    loads[2].wait()
    lane = lax.broadcasted_iota(jnp.int32, (rows, table.shape[2]), 1)
    dense = jnp.zeros((rows, table.shape[2]), F32)
    chosen, strength = jnp.transpose(routes[...]), jnp.transpose(rw[...])
    for k in range(routes.shape[0]):
        dense = dense + jnp.where(lane == chosen[:, k : k + 1], strength[:, k : k + 1], 0.0)
    table[e] = dense
    loads[0].wait()
    pl.semaphore_wait(barrier, len(partners))

    sends = []

    def remote(source, target, send, recv, device, go=True):
        copy = pltpu.make_async_remote_copy(
            src_ref=source,
            dst_ref=target,
            send_sem=send,
            recv_sem=recv,
            device_id=device,
            device_id_type=MESH,
        )
        if go:
            copy.start()
            sends.append(copy)
        return copy

    for step in far_first(groups):
        if step:
            mine = xbuf.at[p, block(e)]
            remote(mine, mine, zs_sem.at[step], zr_sem.at[step], (lax.rem(e + step, groups), p))
    if groups * chips <= 32:
        pieces = [[0]] + [[step] for step in far_first(groups)[::-1] if step]
    else:
        pieces = [list(range(groups))]

    def piece_rows(piece):
        if len(piece) > 1:
            return pl.ds(0, tokens)
        return block(lax.rem(e + groups - piece[0], groups))

    core_next = lax.rem(c + 1, cores)
    for number, piece in enumerate(pieces):
        for step in piece:
            if step:
                theirs = xbuf.at[p, block(lax.rem(e + groups - step, groups))]
                remote(theirs, theirs, zs_sem.at[step], zr_sem.at[step], (e, p), False).wait_recv()
        view = xbuf.at[p, piece_rows(piece)]
        for d in range(chips - 1, 0, -1):
            remote(
                view,
                view,
                ps_sem.at[number, d],
                pr_sem.at[number, d],
                (e, at_chip(flip(q, d, chips), c)),
            )
        remote(view, view, ds_sem.at[number, 0], dr_sem.at[number, 0], (e, at_chip(q, core_next)))
        if number == 0:
            for step in far_first(groups):
                if step:
                    remote(
                        table.at[e],
                        table.at[e],
                        ts_sem.at[step],
                        tr_sem.at[step],
                        (lax.rem(e + step, groups), p),
                    )

    def project(owner, first):
        values = xbuf[owner].astype(F32)
        scaled = (values * gain[:, columns(owner)]).astype(BF16)
        squares = values * values
        partial = squares[:, :128]
        for start in range(128, feats, 128):
            partial = partial + squares[:, start : start + 128]
        for acc, weight in (
            (acc_g, gate_w),
            (acc_u, up_w),
            (acc_sg, sgate_w),
            (acc_su, sup_w),
        ):
            product = lax.dot_general(
                scaled, weight[:, columns(owner)], NT, preferred_element_type=F32
            )
            acc[...] = product if first else acc[...] + product
        acc_ss[...] = partial if first else acc_ss[...] + partial

    for load in loads[3:first_done]:
        load.wait()
    project(p, True)

    def forwarded(d):
        owner = at_chip(unflip(q, d, chips), core_next)
        for number, piece in enumerate(pieces):
            view = xbuf.at[owner, piece_rows(piece)]
            remote(view, view, ds_sem.at[number, d], dr_sem.at[number, d], (e, p), False).wait_recv()
        project(owner, False)

    for d in range(1, chips):
        owner = at_chip(unflip(q, d, chips), c)
        for number, piece in enumerate(pieces):
            view = xbuf.at[owner, piece_rows(piece)]
            remote(view, view, ps_sem.at[number, d], pr_sem.at[number, d], (e, p), False).wait_recv()
            remote(
                view, view, ds_sem.at[number, d], dr_sem.at[number, d], (e, at_chip(q, core_next))
            )
        project(owner, False)
        if d > 1:
            forwarded(d - 2)
    for d in range(max(chips - 2, 0), chips):
        forwarded(d)

    for step in range(1, groups):
        theirs = table.at[lax.rem(e + groups - step, groups)]
        remote(theirs, theirs, ts_sem.at[step], tr_sem.at[step], (e, p), False).wait_recv()

    inv = lax.rsqrt(jnp.sum(acc_ss[...], axis=1, keepdims=True) / (feats * width) + norm_eps)
    tables = table[...].reshape(tokens, table.shape[2])
    lanes = lax.broadcasted_iota(jnp.int32, tables.shape, 1)
    unit = lax.broadcasted_iota(jnp.int32, (tokens, local * units), 1)
    mix = jnp.zeros((tokens, local * units), F32)
    for index in range(local):
        mine = jnp.sum(
            jnp.where(lanes == e * local + index, tables, 0.0), axis=1, keepdims=True
        )
        inside = (unit >= index * units) & (unit < (index + 1) * units)
        mix = jnp.where(inside, mine, mix)

    def swish(v):
        return v / (1.0 + jnp.exp(-v))

    inner = (swish(acc_g[...] * inv) * (acc_u[...] * inv) * mix).astype(BF16)
    shared = swish(acc_sg[...] * inv) * (acc_su[...] * inv)
    if not shared_split:
        row = lax.broadcasted_iota(jnp.int32, shared.shape, 0)
        shared = jnp.where((row >= e * rows) & (row < (e + 1) * rows), shared, 0.0)
    shared = shared.astype(BF16)
    for load in loads[first_done:]:
        load.wait()

    def expand(owner):
        return jnp.dot(
            inner, down_w[:, columns(owner)], preferred_element_type=F32
        ) + jnp.dot(shared, sdown_w[:, columns(owner)], preferred_element_type=F32)

    order = list(range(chips - 1, -1, -1))
    for d in order:
        core_send[d] = expand(at_chip(flip(q, d, chips), core_next)).astype(BF16)
        remote(
            core_send.at[d], core_recv.at[d], cs_sem.at[d], cr_sem.at[d], (e, at_chip(q, core_next))
        )
    if len(pieces) > 1:
        out_pieces = [[step] for step in far_first(groups)]
    else:
        out_pieces = pieces

    def out_rows(piece):
        if len(piece) > 1:
            return pl.ds(0, tokens)
        return block(lax.rem(e + piece[0], groups))

    for d in order:
        value = expand(at_chip(flip(q, d, chips), c))
        remote(
            core_send.at[d], core_recv.at[d], cs_sem.at[d], cr_sem.at[d], (e, p), False
        ).wait_recv()
        value = value + core_recv[d].astype(F32)
        if d == 0:
            total[...] = value
        else:
            plane_send[d] = value.astype(BF16)
        if d == 1:
            for number, piece in enumerate(out_pieces):
                for peer in order[:-1]:
                    remote(
                        plane_send.at[peer, out_rows(piece)],
                        plane_recv.at[peer, out_rows(piece)],
                        qs_sem.at[number, peer],
                        qr_sem.at[number, peer],
                        (e, at_chip(flip(q, peer, chips), c)),
                    )
    for number, piece in enumerate(out_pieces):
        for d in range(1, chips):
            view = plane_recv.at[d, out_rows(piece)]
            remote(view, view, qs_sem.at[number, d], qr_sem.at[number, d], (e, p), False).wait_recv()
        for step in piece:
            span = block(lax.rem(e + step, groups))
            value = total[span, :]
            for d in range(1, chips):
                value = value + plane_recv[d, span, :].astype(F32)
            if step:
                z_send[step] = value.astype(BF16)
                remote(
                    z_send.at[step],
                    z_recv.at[step],
                    ys_sem.at[step],
                    yr_sem.at[step],
                    (lax.rem(e + step, groups), p),
                )
            else:
                total[span, :] = value
    answer = total[block(e), :]
    for step in range(1, groups):
        remote(
            z_send.at[step], z_recv.at[step], ys_sem.at[step], yr_sem.at[step], (e, p), False
        ).wait_recv()
        answer = answer + z_recv[step].astype(F32)
    out_ref[...] = answer.astype(BF16)
    for copy in sends:
        copy.wait_send()


def solution(mesh):
    groups, width = mesh.shape["ep"], mesh.shape["tp"]
    cores = 2

    def step(hidden, gain, routes, rw, gate, up, down, sgate, sup, sdown):
        rows, feats = hidden.shape
        local, units, model = gate.shape
        tokens = rows * groups
        chips = width // cores
        shared_units = sgate.shape[0]
        shared_split = shared_units % (16 * groups) == 0
        split_units = shared_units // groups if shared_split else shared_units
        lanes = -(-local * groups // 128) * 128
        count = groups if groups * chips <= 32 else 1
        dma = pltpu.SemaphoreType.DMA
        any_spec = pl.BlockSpec(memory_space=pl.ANY)
        return pl.pallas_call(
            functools.partial(kernel, groups, width, cores, shared_split),
            out_shape=pltpu.VMEM((rows, feats), BF16),
            in_specs=[any_spec] * 10,
            out_specs=pl.BlockSpec(memory_space=pltpu.VMEM),
            scratch_shapes=[
                pltpu.VMEM((width, tokens, feats), BF16),
                pltpu.VMEM((1, model), F32),
                pltpu.VMEM(routes.shape[::-1], jnp.int32),
                pltpu.VMEM(rw.shape[::-1], F32),
                pltpu.VMEM((groups, rows, lanes), F32),
                pltpu.VMEM((local * units, model), BF16),
                pltpu.VMEM((local * units, model), BF16),
                pltpu.VMEM((local * units, model), BF16),
                pltpu.VMEM((split_units, model), BF16),
                pltpu.VMEM((split_units, model), BF16),
                pltpu.VMEM((split_units, model), BF16),
                pltpu.VMEM((tokens, local * units), F32),
                pltpu.VMEM((tokens, local * units), F32),
                pltpu.VMEM((tokens, split_units), F32),
                pltpu.VMEM((tokens, split_units), F32),
                pltpu.VMEM((tokens, 128), F32),
                pltpu.VMEM((chips, tokens, feats), BF16),
                pltpu.VMEM((chips, tokens, feats), BF16),
                pltpu.VMEM((chips, tokens, feats), BF16),
                pltpu.VMEM((chips, tokens, feats), BF16),
                pltpu.VMEM((tokens, feats), F32),
                pltpu.VMEM((groups, rows, feats), BF16),
                pltpu.VMEM((groups, rows, feats), BF16),
                dma((4 + 3 * local + 3,)),
                dma((groups,)),
                dma((groups,)),
                dma((groups,)),
                dma((groups,)),
                dma((count, chips)),
                dma((count, chips)),
                dma((count, chips)),
                dma((count, chips)),
                dma((chips,)),
                dma((chips,)),
                dma((count, chips)),
                dma((count, chips)),
                dma((groups,)),
                dma((groups,)),
            ],
            compiler_params=pltpu.CompilerParams(
                collective_id=0,
                has_side_effects=True,
                vmem_limit_bytes=60 * 1024 * 1024,
            ),
            name="moe_step",
        )(hidden, gain.reshape(1, -1), routes.T, rw.T, gate, up, down, sgate, sup, sdown)

    in_specs = (
        P("ep", "tp"),
        P(),
        P("ep", None),
        P("ep", None),
        P("ep", "tp", None),
        P("ep", "tp", None),
        P("ep", "tp", None),
        P("tp", None),
        P("tp", None),
        P("tp", None),
    )
    return jax.shard_map(
        step, mesh=mesh, in_specs=in_specs, out_specs=P("ep", "tp"), check_vma=False
    )
```

```python
import functools

import jax
import jax.numpy as jnp
from jax import lax
from jax.experimental import pallas as pl
from jax.experimental.pallas import tpu as pltpu
from jax.sharding import PartitionSpec as P

MESH = pl.DeviceIdType.MESH
norm_eps = 1e-06
NT = (((1,), (1,)), ((), ()))
F32 = jnp.float32
BF16 = jnp.bfloat16


def flip(index, bits, count):
    if count & (count - 1):
        return lax.rem(index + bits, count)
    result, place = 0, 1
    while place < count:
        digit = lax.rem(index // place, 2)
        if (bits // place) % 2:
            digit = 1 - digit
        result = result + digit * place
        place *= 2
    return result


def unflip(index, bits, count):
    if count & (count - 1):
        return lax.rem(index + count - bits, count)
    return flip(index, bits, count)


def far_first(count):
    return sorted(range(count), key=lambda step: -min(step, count - step))


def kernel(
    groups,
    width,
    cores,
    shared_split,
    hidden_hbm,
    gain_hbm,
    routes_hbm,
    rw_hbm,
    gate_hbm,
    up_hbm,
    down_hbm,
    sgate_hbm,
    sup_hbm,
    sdown_hbm,
    out_ref,
    xbuf,
    gain,
    routes,
    rw,
    table,
    gate_w,
    up_w,
    down_w,
    sgate_w,
    sup_w,
    sdown_w,
    acc_g,
    acc_u,
    acc_sg,
    acc_su,
    acc_ss,
    core_send,
    core_recv,
    plane_send,
    plane_recv,
    total,
    z_send,
    z_recv,
    load_sem,
    zs_sem,
    zr_sem,
    ts_sem,
    tr_sem,
    ps_sem,
    pr_sem,
    ds_sem,
    dr_sem,
    cs_sem,
    cr_sem,
    qs_sem,
    qr_sem,
    ys_sem,
    yr_sem,
):
    e = lax.axis_index("ep")
    p = lax.axis_index("tp")
    chips = width // cores
    q, c = p // cores, lax.rem(p, cores)
    rows, feats = hidden_hbm.shape
    tokens = rows * groups
    local, units, _ = gate_hbm.shape
    split_units = sgate_w.shape[0]

    def at_chip(chip, core):
        return chip * cores + core

    def block(index):
        return pl.ds(pl.multiple_of(index * rows, rows), rows)

    def columns(index):
        return pl.ds(pl.multiple_of(index * feats, feats), feats)

    loads = [
        pltpu.make_async_copy(hidden_hbm, xbuf.at[p, block(e)], load_sem.at[0]),
        pltpu.make_async_copy(routes_hbm, routes, load_sem.at[1]),
        pltpu.make_async_copy(rw_hbm, rw, load_sem.at[2]),
        pltpu.make_async_copy(gain_hbm, gain, load_sem.at[3]),
    ]
    part = pl.ds(
        pl.multiple_of(e * split_units, split_units) if shared_split else 0, split_units
    )
    number = len(loads)
    for index in range(local):
        span = pl.ds(index * units, units)
        for source, target in ((gate_hbm, gate_w), (up_hbm, up_w)):
            loads.append(
                pltpu.make_async_copy(source.at[index], target.at[span], load_sem.at[len(loads)])
            )
    for source, target in ((sgate_hbm, sgate_w), (sup_hbm, sup_w)):
        loads.append(pltpu.make_async_copy(source.at[part], target, load_sem.at[len(loads)]))
    first_done = len(loads)
    for index in range(local):
        span = pl.ds(index * units, units)
        loads.append(
            pltpu.make_async_copy(down_hbm.at[index], down_w.at[span], load_sem.at[len(loads)])
        )
    loads.append(pltpu.make_async_copy(sdown_hbm.at[part], sdown_w, load_sem.at[len(loads)]))
    for load in loads:
        load.start()

    barrier = pltpu.get_barrier_semaphore()
    partners = [(lax.rem(e + step, groups), p) for step in range(1, groups)]
    partners += [(e, at_chip(flip(q, d, chips), c)) for d in range(1, chips)]
    partners += [(e, at_chip(q, lax.rem(c + step, cores))) for step in range(1, cores)]
    for partner in partners:
        pl.semaphore_signal(barrier, inc=1, device_id=partner, device_id_type=MESH)

    loads[1].wait()
    loads[2].wait()
    lane = lax.broadcasted_iota(jnp.int32, (rows, table.shape[2]), 1)
    dense = jnp.zeros((rows, table.shape[2]), F32)
    chosen, strength = jnp.transpose(routes[...]), jnp.transpose(rw[...])
    for k in range(routes.shape[0]):
        dense = dense + jnp.where(lane == chosen[:, k : k + 1], strength[:, k : k + 1], 0.0)
    table[e] = dense
    loads[0].wait()
    pl.semaphore_wait(barrier, len(partners))

    sends = []

    def remote(source, target, send, recv, device, go=True):
        copy = pltpu.make_async_remote_copy(
            src_ref=source,
            dst_ref=target,
            send_sem=send,
            recv_sem=recv,
            device_id=device,
            device_id_type=MESH,
        )
        if go:
            copy.start()
            sends.append(copy)
        return copy

    near, far = far_first(groups)[::-1], far_first(groups)
    near, far = [step for step in near if step], [step for step in far if step]
    if groups == 4:
        low, high = (groups - 1 - e) // (groups - 1), e // (groups - 1)
        near = [1 + 2 * low, 3 - low - high, 2 - low + high]
        far = [2 + low - high, 3 - low - high, 1 + 2 * high]

    def own(step):
        return isinstance(step, int) and step == 0

    for step in far:
        if not own(step):
            mine = xbuf.at[p, block(e)]
            remote(mine, mine, zs_sem.at[step], zr_sem.at[step], (lax.rem(e + step, groups), p))
    if groups * chips <= 32:
        pieces = [[0]] + [[step] for step in near]
    else:
        pieces = [list(range(groups))]

    def piece_rows(piece):
        if len(piece) > 1:
            return pl.ds(0, tokens)
        return block(lax.rem(e + groups - piece[0], groups))

    core_next = lax.rem(c + 1, cores)
    for number, piece in enumerate(pieces):
        for step in piece:
            if not own(step):
                theirs = xbuf.at[p, block(lax.rem(e + groups - step, groups))]
                remote(theirs, theirs, zs_sem.at[step], zr_sem.at[step], (e, p), False).wait_recv()
        view = xbuf.at[p, piece_rows(piece)]
        for d in range(chips - 1, 0, -1):
            remote(
                view,
                view,
                ps_sem.at[number, d],
                pr_sem.at[number, d],
                (e, at_chip(flip(q, d, chips), c)),
            )
        remote(view, view, ds_sem.at[number, 0], dr_sem.at[number, 0], (e, at_chip(q, core_next)))
        if number == 0:
            for step in far_first(groups):
                if step:
                    remote(
                        table.at[e],
                        table.at[e],
                        ts_sem.at[step],
                        tr_sem.at[step],
                        (lax.rem(e + step, groups), p),
                    )

    def project(owner, first):
        values = xbuf[owner].astype(F32)
        scaled = (values * gain[:, columns(owner)]).astype(BF16)
        squares = values * values
        partial = squares[:, :128]
        for start in range(128, feats, 128):
            partial = partial + squares[:, start : start + 128]
        for acc, weight in (
            (acc_g, gate_w),
            (acc_u, up_w),
            (acc_sg, sgate_w),
            (acc_su, sup_w),
        ):
            product = lax.dot_general(
                scaled, weight[:, columns(owner)], NT, preferred_element_type=F32
            )
            acc[...] = product if first else acc[...] + product
        acc_ss[...] = partial if first else acc_ss[...] + partial

    for load in loads[3:first_done]:
        load.wait()
    project(p, True)

    def forwarded(d):
        owner = at_chip(unflip(q, d, chips), core_next)
        for number, piece in enumerate(pieces):
            view = xbuf.at[owner, piece_rows(piece)]
            remote(view, view, ds_sem.at[number, d], dr_sem.at[number, d], (e, p), False).wait_recv()
        project(owner, False)

    for d in range(1, chips):
        owner = at_chip(unflip(q, d, chips), c)
        for number, piece in enumerate(pieces):
            view = xbuf.at[owner, piece_rows(piece)]
            remote(view, view, ps_sem.at[number, d], pr_sem.at[number, d], (e, p), False).wait_recv()
            remote(
                view, view, ds_sem.at[number, d], dr_sem.at[number, d], (e, at_chip(q, core_next))
            )
        project(owner, False)
        if d > 1:
            forwarded(d - 2)
    for d in range(max(chips - 2, 0), chips):
        forwarded(d)

    for step in range(1, groups):
        theirs = table.at[lax.rem(e + groups - step, groups)]
        remote(theirs, theirs, ts_sem.at[step], tr_sem.at[step], (e, p), False).wait_recv()

    inv = lax.rsqrt(jnp.sum(acc_ss[...], axis=1, keepdims=True) / (feats * width) + norm_eps)
    tables = table[...].reshape(tokens, table.shape[2])
    lanes = lax.broadcasted_iota(jnp.int32, tables.shape, 1)
    unit = lax.broadcasted_iota(jnp.int32, (tokens, local * units), 1)
    mix = jnp.zeros((tokens, local * units), F32)
    for index in range(local):
        mine = jnp.sum(
            jnp.where(lanes == e * local + index, tables, 0.0), axis=1, keepdims=True
        )
        inside = (unit >= index * units) & (unit < (index + 1) * units)
        mix = jnp.where(inside, mine, mix)

    def swish(v):
        return v / (1.0 + jnp.exp(-v))

    inner = (swish(acc_g[...] * inv) * (acc_u[...] * inv) * mix).astype(BF16)
    shared = swish(acc_sg[...] * inv) * (acc_su[...] * inv)
    if not shared_split:
        row = lax.broadcasted_iota(jnp.int32, shared.shape, 0)
        shared = jnp.where((row >= e * rows) & (row < (e + 1) * rows), shared, 0.0)
    shared = shared.astype(BF16)
    for load in loads[first_done:]:
        load.wait()

    def expand(owner):
        return jnp.dot(
            inner, down_w[:, columns(owner)], preferred_element_type=F32
        ) + jnp.dot(shared, sdown_w[:, columns(owner)], preferred_element_type=F32)

    order = list(range(chips - 1, -1, -1))
    for d in order:
        core_send[d] = expand(at_chip(flip(q, d, chips), core_next)).astype(BF16)
        remote(
            core_send.at[d], core_recv.at[d], cs_sem.at[d], cr_sem.at[d], (e, at_chip(q, core_next))
        )
    if len(pieces) > 1:
        out_pieces = [[step] for step in far] + [[0]]
    else:
        out_pieces = pieces

    def out_rows(piece):
        if len(piece) > 1:
            return pl.ds(0, tokens)
        return block(lax.rem(e + piece[0], groups))

    for d in order:
        value = expand(at_chip(flip(q, d, chips), c))
        remote(
            core_send.at[d], core_recv.at[d], cs_sem.at[d], cr_sem.at[d], (e, p), False
        ).wait_recv()
        value = value + core_recv[d].astype(F32)
        if d == 0:
            total[...] = value
        else:
            plane_send[d] = value.astype(BF16)
        if d == 1:
            for number, piece in enumerate(out_pieces):
                for peer in order[:-1]:
                    remote(
                        plane_send.at[peer, out_rows(piece)],
                        plane_recv.at[peer, out_rows(piece)],
                        qs_sem.at[number, peer],
                        qr_sem.at[number, peer],
                        (e, at_chip(flip(q, peer, chips), c)),
                    )
    for number, piece in enumerate(out_pieces):
        for d in range(1, chips):
            view = plane_recv.at[d, out_rows(piece)]
            remote(view, view, qs_sem.at[number, d], qr_sem.at[number, d], (e, p), False).wait_recv()
        for step in piece:
            span = block(lax.rem(e + step, groups))
            value = total[span, :]
            for d in range(1, chips):
                value = value + plane_recv[d, span, :].astype(F32)
            if not own(step):
                z_send[step] = value.astype(BF16)
                remote(
                    z_send.at[step],
                    z_recv.at[step],
                    ys_sem.at[step],
                    yr_sem.at[step],
                    (lax.rem(e + step, groups), p),
                )
            else:
                total[span, :] = value
    answer = total[block(e), :]
    for step in range(1, groups):
        remote(
            z_send.at[step], z_recv.at[step], ys_sem.at[step], yr_sem.at[step], (e, p), False
        ).wait_recv()
        answer = answer + z_recv[step].astype(F32)
    out_ref[...] = answer.astype(BF16)
    for copy in sends:
        copy.wait_send()


def solution(mesh):
    groups, width = mesh.shape["ep"], mesh.shape["tp"]
    cores = 2

    def step(hidden, gain, routes, rw, gate, up, down, sgate, sup, sdown):
        rows, feats = hidden.shape
        local, units, model = gate.shape
        tokens = rows * groups
        chips = width // cores
        shared_units = sgate.shape[0]
        shared_split = shared_units % (16 * groups) == 0
        split_units = shared_units // groups if shared_split else shared_units
        lanes = -(-local * groups // 128) * 128
        count = groups if groups * chips <= 32 else 1
        dma = pltpu.SemaphoreType.DMA
        any_spec = pl.BlockSpec(memory_space=pl.ANY)
        return pl.pallas_call(
            functools.partial(kernel, groups, width, cores, shared_split),
            out_shape=pltpu.VMEM((rows, feats), BF16),
            in_specs=[any_spec] * 10,
            out_specs=pl.BlockSpec(memory_space=pltpu.VMEM),
            scratch_shapes=[
                pltpu.VMEM((width, tokens, feats), BF16),
                pltpu.VMEM((1, model), F32),
                pltpu.VMEM(routes.shape[::-1], jnp.int32),
                pltpu.VMEM(rw.shape[::-1], F32),
                pltpu.VMEM((groups, rows, lanes), F32),
                pltpu.VMEM((local * units, model), BF16),
                pltpu.VMEM((local * units, model), BF16),
                pltpu.VMEM((local * units, model), BF16),
                pltpu.VMEM((split_units, model), BF16),
                pltpu.VMEM((split_units, model), BF16),
                pltpu.VMEM((split_units, model), BF16),
                pltpu.VMEM((tokens, local * units), F32),
                pltpu.VMEM((tokens, local * units), F32),
                pltpu.VMEM((tokens, split_units), F32),
                pltpu.VMEM((tokens, split_units), F32),
                pltpu.VMEM((tokens, 128), F32),
                pltpu.VMEM((chips, tokens, feats), BF16),
                pltpu.VMEM((chips, tokens, feats), BF16),
                pltpu.VMEM((chips, tokens, feats), BF16),
                pltpu.VMEM((chips, tokens, feats), BF16),
                pltpu.VMEM((tokens, feats), F32),
                pltpu.VMEM((groups, rows, feats), BF16),
                pltpu.VMEM((groups, rows, feats), BF16),
                dma((4 + 3 * local + 3,)),
                dma((groups,)),
                dma((groups,)),
                dma((groups,)),
                dma((groups,)),
                dma((count, chips)),
                dma((count, chips)),
                dma((count, chips)),
                dma((count, chips)),
                dma((chips,)),
                dma((chips,)),
                dma((count, chips)),
                dma((count, chips)),
                dma((groups,)),
                dma((groups,)),
            ],
            compiler_params=pltpu.CompilerParams(
                collective_id=0,
                has_side_effects=True,
                vmem_limit_bytes=60 * 1024 * 1024,
            ),
            name="moe_step",
        )(hidden, gain.reshape(1, -1), routes.T, rw.T, gate, up, down, sgate, sup, sdown)

    in_specs = (
        P("ep", "tp"),
        P(),
        P("ep", None),
        P("ep", None),
        P("ep", "tp", None),
        P("ep", "tp", None),
        P("ep", "tp", None),
        P("tp", None),
        P("tp", None),
        P("tp", None),
    )
    return jax.shard_map(
        step, mesh=mesh, in_specs=in_specs, out_specs=P("ep", "tp"), check_vma=False
    )
```
